512 devices in a mesh: ep: 128 (over z, x, core), tp: 4 (over y).
Axes of the slice: x: 4, y: 4, z: 16, core: 2. Of those that a mesh axis runs over, the one named last changes fastest.
Arguments:
- tokens: bfloat16 [2048, 1024], P('ep'), may hold values from -6 to 6
- old_state: float32 [2048, 4, 128, 128], P('ep', 'tp'), may hold values from -6 to 6
- query_weight: bfloat16 [1024, 512], P(None, 'tp'), may hold values from -0.1875 to 0.1875
- forget_weight: bfloat16 [1024, 512], P(None, 'tp'), may hold values from -0.1875 to 0.1875
- input_weight: bfloat16 [1024, 512], P(None, 'tp'), may hold values from -0.1875 to 0.1875
- lower_bound: float32 [512], P('tp'), may hold values from 0 to 0.9
- head_gain: float32 [4, 128], P('tp'), may hold values from 0.1 to 1.9
- out_weight: bfloat16 [512, 1024], P('tp'), may hold values from -0.25 to 0.25
- mix_gain: float32 [1024], replicated, may hold values from 0.1 to 1.9
- ffn_gain: float32 [1024], replicated, may hold values from 0.1 to 1.9
- group_weight: bfloat16 [1024, 4], replicated, may hold values from -0.1875 to 0.1875
- expert_weight: bfloat16 [1024, 128], replicated, may hold values from -0.1875 to 0.1875
- routes: int32 [2048, 6], P('ep'), may hold values from 0 to 127, all different within a row; in each aligned block of 16 rows (0 to 15, 16 to 31, ...) at most 2 rows name the same one
- gate_weight: bfloat16 [128, 1024, 1024], P('ep', None, 'tp'), may hold values from -0.1875 to 0.1875
- up_weight: bfloat16 [128, 1024, 1024], P('ep', None, 'tp'), may hold values from -0.1875 to 0.1875
- down_weight: bfloat16 [128, 1024, 1024], P('ep', None, 'tp'), may hold values from -0.1875 to 0.1875
Outputs:
- layer_out: bfloat16 [2048, 1024], P('ep', 'tp')
- new_state: float32 [2048, 4, 128, 128], P('ep', 'tp')
The draws below stay inside these ranges and needn't reach their ends.
Inputs may be any that keep to these rules, and one draw needn't show every extreme that they name: `routes`: each row names 6 different experts. In each aligned block of 16 rows (the rows of one device) no expert is named more than 2 times, a bound that some block reaches.
All inputs are finite; a program needn't handle non-finite values.
Results may differ from the reference program's by a relative error of at most 0.011.
Values may be sent and summed in bfloat16 or wider, within the bound.
A program may use at most 64 MiB of HBM per device.

```python
import math
import jax
import jax.numpy as jnp
import numpy as np
from jax import lax

D = 1024
HEADS = 4
HEAD_DIM = 128
FF = 1024
GROUPS = 4
TOPK = 6
SEQ_DEV = 16
HG = 512
EXPERTS = 128
CAP = 2
TOKENS = 2048
N_EP = 128
N_TP = 4


def block_scale(stream_key, dims, pieces, smallest, largest):
    level, own = 1.0, jax.random.fold_in(stream_key, 6)
    for axis_at, parts in pieces:
        draws = jnp.exp(jax.random.uniform(jax.random.fold_in(own, axis_at), (parts,), jnp.float32, smallest / len(pieces), largest / len(pieces)))
        level = level * jnp.repeat(draws, dims[axis_at] // parts).reshape([-1 if axis == axis_at else 1 for axis in range(len(dims))])
    return level


def assign_block(rng, own, number, rows, amount, top, reach, skew):
    order = jax.random.permutation(rng, amount)
    crowded, common = shares(amount, rows * top, reach, skew, True), shares(amount, rows * top, reach, skew, False)
    places = jnp.arange(amount)

    def named(lengths, offset_by):
        used = int((lengths > 0).sum())
        fixed = max(1, used // 4)
        moved = fixed + (places - fixed + offset_by * (used - fixed)) % max(1, amount - fixed)
        return jnp.zeros((amount,), jnp.int32).at[order[jnp.where(places < fixed, places, moved)]].set(jnp.asarray(lengths, jnp.int32))

    lengths = jnp.where(number % 4 == 0, named(crowded, number // 4), named(common, number - number // 4 - 1))
    mixed = jax.random.permutation(jax.random.fold_in(own, 3), amount)
    source_of, receiver = mixed[0:amount // 2 * 2:2], mixed[1:amount // 2 * 2:2]
    margin = jnp.minimum(lengths[source_of] - 1, reach - lengths[receiver]) // 2
    margin = jnp.where((source_of == order[0]) | (receiver == order[0]) | (lengths[receiver] == 0), 0, jnp.maximum(margin, 0))
    moved = jax.random.randint(jax.random.fold_in(own, 4), (amount // 2,), 0, 1 << 20) % (margin + 1)
    lengths = lengths.at[source_of].add(-moved).at[receiver].add(moved)
    members = jnp.searchsorted(jnp.cumsum(lengths), jnp.arange(rows * top), side="right").astype(jnp.int32)
    table = members.reshape(top, rows).T
    table = table[jax.random.permutation(jax.random.fold_in(own, 1), rows)]
    offset_by = jax.random.randint(jax.random.fold_in(own, 2), (rows, 1), 0, top)
    return jnp.take_along_axis(table, (jnp.arange(top)[None, :] + offset_by) % top, axis=1)


def shares(number_of, total, bound, skew, full):
    portions = [(1 << 20) // math.isqrt(standing ** skew) + 1 for standing in range(1, number_of + 1)]
    largest = bound if full else min(bound, max(-(-total // number_of), total * portions[0] // sum(portions)))
    least = 1 if total - largest >= number_of - 1 else 0
    given, rest = [largest] + [least] * (number_of - 1), total - largest - least * (number_of - 1)
    while rest > 0:
        candidates = [i for i in range(1, number_of) if given[i] < largest] or [i for i in range(1, number_of) if given[i] < bound]
        whole, left = sum([portions[i] for i in candidates]), rest
        for i in candidates:
            more = min(bound - given[i], max(1, left * portions[i] // whole), rest)
            given[i] = given[i] + more
            rest = rest - more
    return np.array(given)


def gaussian(stream_key, shape, width, most, pieces=(), kind=jnp.bfloat16):
    level = block_scale(stream_key, shape, pieces, -0.22, 0.18) if pieces else 1.0
    values = jax.random.normal(stream_key, shape, jnp.float32) * width * level
    return jnp.minimum(jnp.maximum(values, -most), most).astype(kind)


def setup_inputs(seed: int = 0) -> dict:
    splits = jax.random.split(jax.random.key(seed), 17)
    tokens = gaussian(splits[0], (TOKENS, D), 1.0, 6.0, ((0, 128),))
    old_state = gaussian(splits[1], (TOKENS, HEADS, HEAD_DIM, HEAD_DIM), 1.0, 6.0, ((0, 128), (1, 4)), jnp.float32)
    query_weight = gaussian(splits[2], (D, HG), D ** -0.5, 0.1875, ((1, 4),))
    forget_weight = gaussian(splits[3], (D, HG), D ** -0.5, 0.1875, ((1, 4),))
    input_weight = gaussian(splits[4], (D, HG), D ** -0.5, 0.1875, ((1, 4),))
    lower_bound = jnp.clip(0.9 * jax.random.uniform(splits[5], (HG,), jnp.float32) ** block_scale(splits[5], (HG,), ((0, 4),), -0.2, 0.2), 0.0, 0.9)
    head_gain = jnp.clip(1.0 + 0.18 * jax.random.normal(splits[6], (HEADS, HEAD_DIM), jnp.float32), 0.1, 1.9)
    out_weight = gaussian(splits[7], (HG, D), HG ** -0.5, 0.25, ((0, 4),))
    mix_gain = jnp.clip(1.0 + 0.18 * jax.random.normal(splits[8], (D,), jnp.float32), 0.1, 1.9)
    ffn_gain = jnp.clip(1.0 + 0.18 * jax.random.normal(splits[9], (D,), jnp.float32), 0.1, 1.9)
    group_weight = gaussian(splits[10], (D, GROUPS), D ** -0.5, 0.1875)
    expert_weight = gaussian(splits[11], (D, EXPERTS), D ** -0.5, 0.1875)
    routes_keys = jax.random.split(jax.random.fold_in(splits[12], 1), TOKENS // SEQ_DEV)
    routes_turns = jax.random.permutation(jax.random.fold_in(splits[12], 3), TOKENS // SEQ_DEV)
    routes = jax.vmap(lambda own, number: assign_block(jax.random.fold_in(splits[12], 2), own, number, SEQ_DEV, EXPERTS, TOPK, CAP, 2))(routes_keys, routes_turns).reshape((TOKENS, TOPK))
    gate_weight = gaussian(splits[13], (EXPERTS, D, FF), D ** -0.5, 0.1875, ((0, 128), (2, 4)))
    up_weight = gaussian(splits[14], (EXPERTS, D, FF), D ** -0.5, 0.1875, ((0, 128), (2, 4)))
    down_weight = gaussian(splits[15], (EXPERTS, FF, D), FF ** -0.5, 0.1875, ((0, 128), (2, 4)))
    return {"tokens": tokens, "old_state": old_state, "query_weight": query_weight, "forget_weight": forget_weight, "input_weight": input_weight, "lower_bound": lower_bound, "head_gain": head_gain, "out_weight": out_weight, "mix_gain": mix_gain, "ffn_gain": ffn_gain, "group_weight": group_weight, "expert_weight": expert_weight, "routes": routes, "gate_weight": gate_weight, "up_weight": up_weight, "down_weight": down_weight}


epsilon = 1e-06

def scaled_rms(values, gain):
    return values * lax.rsqrt(lax.optimization_barrier(jnp.mean(values * values, axis=-1, keepdims=True)) + epsilon) * gain

def block_slots(route_blocks):
    hits = (route_blocks[:, :, None] == jnp.arange(EXPERTS, dtype=jnp.int32)[None, None, :]).astype(jnp.int32)
    before = jnp.cumsum(hits, axis=1) - hits
    return lax.optimization_barrier(jnp.sum(hits * before, axis=2))

def reference(tokens, old_state, query_weight, forget_weight, input_weight, lower_bound, head_gain, out_weight, mix_gain, ffn_gain, group_weight, expert_weight, routes, gate_weight, up_weight, down_weight):
    resident = tokens.astype(jnp.float32)
    normed = scaled_rms(resident, mix_gain).astype(jnp.bfloat16)
    query_pre = jnp.dot(normed, query_weight, preferred_element_type=jnp.float32)
    forget_pre = jnp.dot(normed, forget_weight, preferred_element_type=jnp.float32)
    input_pre = jnp.dot(normed, input_weight, preferred_element_type=jnp.float32)
    query = jax.nn.silu(query_pre).reshape(TOKENS, HEADS, HEAD_DIM)
    forget = (lower_bound + (1.0 - lower_bound) * jax.nn.sigmoid(forget_pre)).reshape(TOKENS, HEADS, HEAD_DIM)
    value = input_pre.reshape(TOKENS, HEADS, HEAD_DIM)
    new_state = forget[..., None] * old_state + (1.0 - forget)[..., None] * value[:, :, None, :]
    readout = lax.optimization_barrier(jnp.sum(new_state * query[..., None], axis=2))
    head_out = scaled_rms(readout, head_gain).astype(jnp.bfloat16).reshape(TOKENS, HEADS * HEAD_DIM)
    width_block = HEADS * HEAD_DIM // N_TP
    mixed = jnp.zeros((TOKENS, D), jnp.float32)
    for index in range(N_TP):
        lower = index * width_block
        partial_sum = jnp.dot(head_out[:, lower:lower + width_block], out_weight[lower:lower + width_block], preferred_element_type=jnp.float32)
        rounded = lax.optimization_barrier(partial_sum.astype(jnp.bfloat16))
        mixed = mixed + rounded.astype(jnp.float32)
    mixed_rounded = lax.optimization_barrier(mixed.astype(jnp.bfloat16))
    residual = (resident + mixed_rounded.astype(jnp.float32)).astype(jnp.bfloat16)
    ffn_in = scaled_rms(residual.astype(jnp.float32), ffn_gain).astype(jnp.bfloat16)
    group_raw = jnp.exp(jnp.dot(ffn_in, group_weight, preferred_element_type=jnp.float32))
    group_prob = group_raw / lax.optimization_barrier(jnp.sum(group_raw, axis=-1, keepdims=True))
    per_group = EXPERTS // GROUPS
    expert_raw = jnp.exp(jnp.dot(ffn_in, expert_weight, preferred_element_type=jnp.float32)).reshape(TOKENS, GROUPS, per_group)
    expert_prob = expert_raw / lax.optimization_barrier(jnp.sum(expert_raw, axis=-1, keepdims=True)) * group_prob[:, :, None]
    expert_prob = expert_prob.reshape(TOKENS, EXPERTS)
    chosen = routes[:, :, None] == jnp.arange(EXPERTS, dtype=jnp.int32)[None, None, :]
    weight = lax.optimization_barrier(jnp.sum(jnp.where(chosen, expert_prob[:, None, :], 0.0), axis=-1))
    gate = weight / lax.optimization_barrier(jnp.sum(weight, axis=-1, keepdims=True))
    rows_per = N_EP * CAP
    slots = block_slots(routes.reshape(N_EP, SEQ_DEV * TOPK)).reshape(-1)
    flat = routes.reshape(-1)
    owner = jnp.arange(TOKENS * TOPK, dtype=jnp.int32) // (SEQ_DEV * TOPK)
    target = (flat * rows_per + owner * CAP + slots).astype(jnp.int32)
    token_of = jnp.arange(TOKENS * TOPK, dtype=jnp.int32) // TOPK
    buffer = jnp.zeros((EXPERTS * rows_per, D), jnp.bfloat16).at[target].set(ffn_in[token_of])
    buffer = buffer.reshape(EXPERTS, rows_per, D)

    def expert(inputs):
        rows, gate_part, up_part, down_part = inputs
        hidden = (jax.nn.silu(jnp.dot(rows, gate_part, preferred_element_type=jnp.float32)) * jnp.dot(rows, up_part, preferred_element_type=jnp.float32)).astype(jnp.bfloat16)
        return jnp.dot(hidden, down_part, preferred_element_type=jnp.float32).astype(jnp.bfloat16)
    produced = lax.map(expert, (buffer, gate_weight, up_weight, down_weight)).reshape(EXPERTS * rows_per, D)
    picked = produced[target].astype(jnp.float32).reshape(TOKENS, TOPK, D)
    mixture = lax.optimization_barrier(jnp.sum(gate[:, :, None] * picked, axis=1))
    layer_out = (residual.astype(jnp.float32) + mixture).astype(jnp.bfloat16)
    return (layer_out, new_state)
```

```python
import jax
import jax.numpy as jnp
from jax import lax
from jax.experimental import pallas as pl
from jax.experimental.pallas import tpu as pltpu
from jax.sharding import PartitionSpec as P

epsilon = 1e-06
MESH = pl.DeviceIdType.MESH
BF = jnp.bfloat16
F32 = jnp.float32

DIST = [0] + [(p + 1) // 2 if p % 2 else 16 - p // 2 for p in range(1, 16)]
BACK = [DIST.index((16 - d) % 16) for d in DIST]
FAR = list(range(15, 0, -1))
CHUNKS = [(12, 16), (8, 12), (4, 8), (0, 4)]
GROUP = [j for j in (4, 5, 2, 3, 6, 7, 1)]


def group_back(j):
    return ((4 - j // 2) % 4) * 2 + j % 2


def kernel(
    tok_h,
    st_h,
    wq_h,
    wf_h,
    wi_h,
    lb_h,
    hg_h,
    wo_h,
    mg_h,
    fg_h,
    gw_h,
    ew_h,
    rt_h,
    wg_h,
    wu_h,
    wd_h,
    out_ref,
    ns_h,
    tok,
    st,
    wq,
    wf,
    wi,
    lb,
    hg,
    wo,
    mg,
    fg,
    gw,
    ew,
    rt,
    wg,
    wu,
    wd,
    hp,
    rs,
    d1,
    cb,
    res,
    gb,
    d2s,
    xb,
    hb,
    pb,
    rr,
    r2s,
    r2r,
    lsem,
    nsem,
    rs_s,
    rs_r,
    d1_s,
    d1_r,
    cb_s,
    cb_r,
    re_s,
    re_r,
    gb_s,
    gb_r,
    d2_s,
    d2_r,
    yf_s,
    yf_r,
    hb_s,
    hb_r,
    r1_s,
    r1_r,
    r2_ss,
    r2_rs,
    k1,
    k2,
    k3,
):
    e = lax.axis_index("ep")
    y = lax.axis_index("tp")
    c = lax.rem(e, 2)
    x = lax.rem(e // 2, 4)
    z = e // 8
    g = lax.rem(e, 8)

    def at_y(d):
        return (e, lax.rem(y + d, 4))

    def at_g(j):
        x2 = lax.rem(x + j // 2, 4)
        c2 = lax.rem(c + j % 2, 2)
        return ((z * 4 + x2) * 2 + c2, y)

    def at_z(d):
        return (lax.rem(z + d, 16) * 8 + g, y)

    def remote(src, dst, ss, sr, dev):
        return pltpu.make_async_remote_copy(
            src_ref=src, dst_ref=dst, send_sem=ss, recv_sem=sr, device_id=dev, device_id_type=MESH
        )

    barrier = pltpu.get_barrier_semaphore()
    for dev in [at_z(1), at_z(15)] + [at_g(j) for j in GROUP] + [at_y(d) for d in (2, 1, 3)]:
        pl.semaphore_signal(barrier, inc=1, device_id=dev, device_id_type=MESH)

    loads = {}
    pairs = [
        (tok_h, tok),
        (mg_h, mg),
        (wq_h, wq),
        (wf_h, wf),
        (wi_h, wi),
        (lb_h, lb),
        (st_h, st),
        (hg_h, hg),
        (wo_h, wo),
        (rt_h, rt),
        (fg_h, fg),
        (gw_h, gw),
        (ew_h, ew),
        (wg_h, wg),
        (wu_h, wu),
        (wd_h, wd),
    ]
    for i, (src, dst) in enumerate(pairs):
        loads[i] = pltpu.make_async_copy(src, dst, lsem.at[i])
        loads[i].start()

    sends = []

    for i in range(6):
        loads[i].wait()
    t32 = tok[...].astype(F32)
    normed = (
        t32 * lax.rsqrt(jnp.mean(t32 * t32, axis=-1, keepdims=True) + epsilon) * mg[...]
    ).astype(BF)
    q_pre = jnp.dot(normed, wq[...], preferred_element_type=F32)
    f_pre = jnp.dot(normed, wf[...], preferred_element_type=F32)
    value = jnp.dot(normed, wi[...], preferred_element_type=F32)
    query = q_pre * jax.nn.sigmoid(q_pre)
    forget = lb[...] + (1.0 - lb[...]) * jax.nn.sigmoid(f_pre)
    f_t = forget.T
    q_t = query.T
    loads[6].wait()
    rows = []
    for t in range(16):
        f_col = f_t[:, t : t + 1]
        new = f_col * st[t] + (1.0 - f_col) * value[t : t + 1, :]
        st[t] = new
        rows.append(jnp.sum(new * q_t[:, t : t + 1], axis=0, keepdims=True))
    new_copy = pltpu.make_async_copy(st, ns_h, nsem)
    new_copy.start()
    readout = jnp.concatenate(rows, axis=0)
    for i in range(7, 10):
        loads[i].wait()
    head_out = (
        readout
        * lax.rsqrt(jnp.mean(readout * readout, axis=-1, keepdims=True) + epsilon)
        * hg[...]
    ).astype(BF)
    part = jnp.dot(head_out, wo[...], preferred_element_type=F32).astype(BF)
    for b in range(4):
        hp[b] = part[:, b * 256 : (b + 1) * 256]

    lane = lax.broadcasted_iota(jnp.int32, (16, 128), 1)
    hits = jnp.zeros((16, 128), F32)
    routes = rt[...]
    for k in range(6):
        hits = hits + jnp.where(routes[:, k : k + 1] == lane, 1.0, 0.0)
    below = lax.broadcasted_iota(jnp.int32, (16, 16), 0) > lax.broadcasted_iota(
        jnp.int32, (16, 16), 1
    )
    before = jnp.dot(
        jnp.where(below, 1.0, 0.0).astype(BF), hits.astype(BF), preferred_element_type=F32
    )
    cb[0:16, :] = (hits * (1.0 + before)).astype(BF)

    pl.semaphore_wait(barrier, 12)
    for d in (1, 15):
        pl.semaphore_signal(k1, inc=1, device_id=at_z(d), device_id_type=MESH)

    for d in (2, 1, 3):
        to = lax.rem(y + d, 4)
        cp = remote(hp.at[to], rs.at[4 - d], rs_s.at[d], rs_r.at[4 - d], at_y(d))
        cp.start()
        sends.append(cp)
    own = slice(0, 16)
    for j in GROUP:
        b = group_back(j)
        cp = remote(cb.at[own], cb.at[pl.ds(b * 16, 16)], cb_s.at[j], cb_r.at[b], at_g(j))
        cp.start()
        sends.append(cp)
    pl.semaphore_wait(k1, 2)
    for d in (2, 14):
        pl.semaphore_signal(k2, inc=1, device_id=at_z(d), device_id_type=MESH)
    mixed = hp[y].astype(F32)
    for d in (1, 3, 2):
        remote(hp.at[0], rs.at[d], rs_s.at[d], rs_r.at[d], at_y(d)).wait_recv()
        mixed = mixed + rs[d].astype(F32)
    resident = tok[:, pl.ds(pl.multiple_of(y * 256, 256), 256)].astype(F32)
    resid = (resident + mixed.astype(BF).astype(F32)).astype(BF)
    d1[own, :] = resid

    for j in GROUP:
        b = group_back(j)
        cp = remote(d1.at[own], d1.at[pl.ds(b * 16, 16)], d1_s.at[j], d1_r.at[b], at_g(j))
        cp.start()
        sends.append(cp)
    res[y] = resid
    for d in (2, 1, 3):
        cp = remote(d1.at[own], res.at[y], re_s.at[d], re_r.at[4 - d], at_y(d))
        cp.start()
        sends.append(cp)

    def blocks(shape, axis):
        index = lax.broadcasted_iota(jnp.int32, shape, axis)
        p = lax.shift_right_logical(index, 4)
        half = lax.shift_right_logical(p, 1)
        dist = jnp.where((p & 1) == 1, half + 1, (16 - half) & 15)
        expert = ((z + dist) & 15) * 8 + g
        return expert, lax.shift_right_logical(index, 1) & 7, (index & 1).astype(F32) + 1.0

    expert, source, want = blocks((256, 128), 0)
    along = lax.broadcasted_iota(jnp.int32, (256, 128), 1)
    sel = jnp.where(expert == along, 1.0, 0.0).astype(BF)
    for j in range(1, 8):
        remote(
            cb.at[own], cb.at[pl.ds(j * 16, 16)], cb_s.at[j], cb_r.at[j], at_g(j)
        ).wait_recv()
    codes = cb[...]
    nt = (((1,), (1,)), ((), ()))
    found = lax.dot_general(sel, codes, nt, preferred_element_type=F32)
    spread = jnp.where(
        (found == want) & (source == lax.shift_right_logical(along, 4)), 1.0, 0.0
    ).astype(BF)
    pl.semaphore_wait(k2, 2)
    for d in (4, 12):
        pl.semaphore_signal(k3, inc=1, device_id=at_z(d), device_id_type=MESH)
    for j in range(1, 8):
        remote(
            d1.at[own], d1.at[pl.ds(j * 16, 16)], d1_s.at[j], d1_r.at[j], at_g(j)
        ).wait_recv()
    d2s[...] = jnp.dot(spread, d1[...], preferred_element_type=F32).astype(BF)
    pl.semaphore_wait(k3, 2)

    def rows_of(p):
        return pl.ds(p * 16, 16)

    for p in FAR:
        cp = remote(
            d2s.at[rows_of(p)],
            xb.at[y, rows_of(BACK[p])],
            d2_s.at[p],
            d2_r.at[BACK[p]],
            at_z(DIST[p]),
        )
        cp.start()
        sends.append(cp)
    xb[y, 0:16, :] = d2s[0:16, :]

    def forward(p):
        for d in (2, 1, 3):
            cp = remote(
                xb.at[y, rows_of(p)],
                xb.at[y, rows_of(p)],
                yf_s.at[p * 4 + d],
                yf_r.at[p * 4 + 4 - d],
                at_y(d),
            )
            cp.start()
            sends.append(cp)

    forward(0)

    for d in (1, 3, 2):
        remote(
            d1.at[own], res.at[lax.rem(y + d, 4)], re_s.at[d], re_r.at[d], at_y(d)
        ).wait_recv()
    for i in range(10, 13):
        loads[i].wait()
    gain = fg[...]
    r32 = jnp.concatenate([res[b] for b in range(4)], axis=1).astype(F32)
    ffn_in = (
        r32 * lax.rsqrt(jnp.mean(r32 * r32, axis=-1, keepdims=True) + epsilon) * gain
    ).astype(BF)
    group_raw = jnp.exp(jnp.dot(ffn_in, gw[...], preferred_element_type=F32))
    group_prob = group_raw / jnp.sum(group_raw, axis=-1, keepdims=True)
    raw = jnp.exp(jnp.dot(ffn_in, ew[...], preferred_element_type=F32))
    member = lax.shift_right_logical(lane, 5)
    total = jnp.zeros((16, 128), F32)
    prior = jnp.zeros((16, 128), F32)
    for k in range(4):
        mine = member == k
        total = jnp.where(
            mine, jnp.sum(jnp.where(mine, raw, 0.0), axis=-1, keepdims=True), total
        )
        prior = jnp.where(mine, group_prob[:, k : k + 1], prior)
    weight = jnp.where(hits > 0.0, raw / total * prior, 0.0)
    gate = weight / jnp.sum(weight, axis=-1, keepdims=True)
    gate_hi = gate.astype(BF)
    gb[0, 0:16, :] = gate_hi
    gb[1, 0:16, :] = (gate - gate_hi.astype(F32)).astype(BF)
    for j in GROUP:
        b = group_back(j)
        cp = remote(
            gb.at[:, own], gb.at[:, pl.ds(b * 16, 16)], gb_s.at[j], gb_r.at[b], at_g(j)
        )
        cp.start()
        sends.append(cp)

    for p in FAR:
        remote(
            d2s.at[rows_of(p)], xb.at[y, rows_of(p)], d2_s.at[p], d2_r.at[p], at_z(DIST[p])
        ).wait_recv()
        forward(p)

    for i in range(13, 16):
        loads[i].wait()

    def wait_rows(lo, hi):
        for p in range(lo, hi):
            for d in (1, 3, 2):
                at = xb.at[lax.rem(y + d, 4), rows_of(p)]
                remote(at, at, yf_s.at[p * 4 + d], yf_r.at[p * 4 + d], at_y(d)).wait_recv()

    for n, (lo, hi) in enumerate(CHUNKS):
        wait_rows(lo, hi)
        span = slice(lo * 16, hi * 16)
        a32 = jnp.concatenate([xb[b, span, :] for b in range(4)], axis=1).astype(F32)
        rows_in = (
            a32 * lax.rsqrt(jnp.mean(a32 * a32, axis=-1, keepdims=True) + epsilon) * gain
        ).astype(BF)
        gate_hidden = jnp.dot(rows_in, wg[...], preferred_element_type=F32)
        up_hidden = jnp.dot(rows_in, wu[...], preferred_element_type=F32)
        hb[y, span, :] = (gate_hidden * jax.nn.sigmoid(gate_hidden) * up_hidden).astype(BF)
        for d in (2, 1, 3):
            cp = remote(
                hb.at[y, span],
                hb.at[y, span],
                hb_s.at[n * 4 + d],
                hb_r.at[n * 4 + 4 - d],
                at_y(d),
            )
            cp.start()
            sends.append(cp)

    for j in range(1, 8):
        remote(
            gb.at[:, own], gb.at[:, pl.ds(j * 16, 16)], gb_s.at[j], gb_r.at[j], at_g(j)
        ).wait_recv()
    _, source_t, want_t = blocks((128, 256), 1)
    token_t = lax.shift_right_logical(lax.broadcasted_iota(jnp.int32, (128, 256), 0), 4)
    found_t = lax.dot_general(codes, sel, nt, preferred_element_type=F32)
    here = (found_t == want_t) & (source_t == token_t)
    mix_hi = jnp.where(
        here, lax.dot_general(gb[0], sel, nt, preferred_element_type=F32), 0.0
    ).astype(BF)
    mix_lo = jnp.where(
        here, lax.dot_general(gb[1], sel, nt, preferred_element_type=F32), 0.0
    ).astype(BF)

    for n, (lo, hi) in enumerate(CHUNKS):
        span = slice(lo * 16, hi * 16)
        for d in (1, 3, 2):
            at = hb.at[lax.rem(y + d, 4), span]
            remote(at, at, hb_s.at[n * 4 + d], hb_r.at[n * 4 + d], at_y(d)).wait_recv()
        hidden = jnp.concatenate([hb[b, span, :] for b in range(4)], axis=1)
        pb[span, :] = jnp.dot(hidden, wd[...], preferred_element_type=F32).astype(BF)
        for p in range(hi - 1, lo - 1, -1):
            if p:
                cp = remote(
                    pb.at[rows_of(p)],
                    rr.at[rows_of(BACK[p])],
                    r1_s.at[p],
                    r1_r.at[BACK[p]],
                    at_z(DIST[p]),
                )
                cp.start()
                sends.append(cp)
    rr[0:16, :] = pb[0:16, :]

    for p in range(1, 16):
        remote(
            pb.at[rows_of(p)], rr.at[rows_of(p)], r1_s.at[p], r1_r.at[p], at_z(DIST[p])
        ).wait_recv()
    back = rr[...]
    sums = jnp.dot(mix_hi, back, preferred_element_type=F32) + jnp.dot(
        mix_lo, back, preferred_element_type=F32
    )
    r2s[...] = sums.astype(BF)
    for j in GROUP:
        b = group_back(j)
        cp = remote(
            r2s.at[pl.ds(j * 16, 16)], r2r.at[pl.ds(b * 16, 16)], r2_ss.at[j], r2_rs.at[b], at_g(j)
        )
        cp.start()
        sends.append(cp)
    mixture = sums[0:16, :]
    for j in range(1, 8):
        remote(
            r2s.at[pl.ds(j * 16, 16)], r2r.at[pl.ds(j * 16, 16)], r2_ss.at[j], r2_rs.at[j], at_g(j)
        ).wait_recv()
        mixture = mixture + r2r[j * 16 : (j + 1) * 16, :].astype(F32)
    out_ref[...] = (d1[own, :].astype(F32) + mixture).astype(BF)
    new_copy.wait()
    for cp in sends:
        cp.wait_send()


def local(
    tokens,
    old_state,
    query_weight,
    forget_weight,
    input_weight,
    lower_bound,
    head_gain,
    out_weight,
    mix_gain,
    ffn_gain,
    group_weight,
    expert_weight,
    routes,
    gate_weight,
    up_weight,
    down_weight,
):
    operands = (
        tokens,
        old_state.reshape(16, 128, 128),
        query_weight,
        forget_weight,
        input_weight,
        lower_bound.reshape(1, 128),
        head_gain,
        out_weight,
        mix_gain.reshape(1, 1024),
        ffn_gain.reshape(1, 1024),
        group_weight,
        expert_weight,
        routes,
        gate_weight.reshape(1024, 256),
        up_weight.reshape(1024, 256),
        down_weight.reshape(1024, 256),
    )
    dma = pltpu.SemaphoreType.DMA
    layer_out, new_state = pl.pallas_call(
        kernel,
        name="layer",
        out_shape=(
            jax.ShapeDtypeStruct((16, 256), BF),
            jax.ShapeDtypeStruct((16, 128, 128), F32),
        ),
        in_specs=[pl.BlockSpec(memory_space=pl.ANY)] * 16,
        out_specs=(pl.BlockSpec(memory_space=pltpu.VMEM), pl.BlockSpec(memory_space=pl.ANY)),
        scratch_shapes=[pltpu.VMEM(a.shape, a.dtype) for a in operands]
        + [
            pltpu.VMEM((4, 16, 256), BF),
            pltpu.VMEM((4, 16, 256), BF),
            pltpu.VMEM((128, 256), BF),
            pltpu.VMEM((128, 128), BF),
            pltpu.VMEM((4, 16, 256), BF),
            pltpu.VMEM((2, 128, 128), BF),
            pltpu.VMEM((256, 256), BF),
            pltpu.VMEM((4, 256, 256), BF),
            pltpu.VMEM((4, 256, 256), BF),
            pltpu.VMEM((256, 256), BF),
            pltpu.VMEM((256, 256), BF),
            pltpu.VMEM((128, 256), BF),
            pltpu.VMEM((128, 256), BF),
            dma((16,)),
            dma(()),
        ]
        + [dma((4,))] * 2
        + [dma((8,))] * 4
        + [dma((4,))] * 2
        + [dma((8,))] * 2
        + [dma((16,))] * 2
        + [dma((64,))] * 2
        + [dma((16,))] * 2
        + [dma((16,))] * 2
        + [dma((8,))] * 2
        + [pltpu.SemaphoreType.REGULAR] * 3,
        compiler_params=pltpu.CompilerParams(collective_id=0, has_side_effects=True),
    )(*operands)
    return layer_out, new_state.reshape(16, 1, 128, 128)


def solution(mesh):
    in_specs = (
        P("ep", None),
        P("ep", "tp", None, None),
        P(None, "tp"),
        P(None, "tp"),
        P(None, "tp"),
        P("tp"),
        P("tp", None),
        P("tp", None),
        P(),
        P(),
        P(),
        P(),
        P("ep", None),
        P("ep", None, "tp"),
        P("ep", None, "tp"),
        P("ep", None, "tp"),
    )
    out_specs = (P("ep", "tp"), P("ep", "tp", None, None))
    return jax.shard_map(local, mesh=mesh, in_specs=in_specs, out_specs=out_specs, check_vma=False)
```

```python
import jax
import jax.numpy as jnp
from jax import lax
from jax.experimental import pallas as pl
from jax.experimental.pallas import tpu as pltpu
from jax.sharding import PartitionSpec as P

epsilon = 1e-06
MESH = pl.DeviceIdType.MESH
BF = jnp.bfloat16
F32 = jnp.float32

DIST = [0] + [(p + 1) // 2 if p % 2 else 16 - p // 2 for p in range(1, 16)]
BACK = [DIST.index((16 - d) % 16) for d in DIST]
FAR = list(range(15, 0, -1))
ARRIVE = [8, 7, 6, 5, 4, 3, 2, 1, 0, 15, 14, 13, 12, 11, 10, 9]
CHUNKS = [(4, 9), (0, 4), (13, 16), (9, 13)]
GROUP = [4, 5, 2, 3, 6, 7, 1]


def hops(p, j):
    return min(DIST[p], 16 - DIST[p]) + min(j // 2, 4 - j // 2)


ORDER = sorted(
    [(p, j) for p in range(16) for j in range(8) if p or j], key=lambda at: -hops(*at)
)


def group_back(j):
    return ((4 - j // 2) % 4) * 2 + j % 2


def kernel(
    tok_h,
    st_h,
    wq_h,
    wf_h,
    wi_h,
    lb_h,
    hg_h,
    wo_h,
    mg_h,
    fg_h,
    gw_h,
    ew_h,
    rt_h,
    wg_h,
    wu_h,
    wd_h,
    out_ref,
    ns_ref,
    tok,
    st,
    wq,
    wf,
    wi,
    lb,
    hg,
    wo,
    mg,
    fg,
    gw,
    ew,
    rt,
    wg,
    wu,
    wd,
    hp,
    rs,
    d1,
    res,
    d2s,
    xb,
    hb,
    pb,
    rr,
    lsem,
    rs_s,
    rs_r,
    re_s,
    re_r,
    d2_s,
    d2_r,
    yf_s,
    yf_r,
    hb_s,
    hb_r,
    r1_s,
    r1_r,
    k1,
    k2,
):
    e = lax.axis_index("ep")
    y = lax.axis_index("tp")
    c = lax.rem(e, 2)
    x = lax.rem(e // 2, 4)
    z = e // 8
    g = lax.rem(e, 8)

    def at_y(d):
        return (e, lax.rem(y + d, 4))

    def at_g(j):
        x2 = lax.rem(x + j // 2, 4)
        c2 = lax.rem(c + j % 2, 2)
        return ((z * 4 + x2) * 2 + c2, y)

    def at_z(d):
        return (lax.rem(z + d, 16) * 8 + g, y)

    def remote(src, dst, ss, sr, dev):
        return pltpu.make_async_remote_copy(
            src_ref=src, dst_ref=dst, send_sem=ss, recv_sem=sr, device_id=dev, device_id_type=MESH
        )

    barrier = pltpu.get_barrier_semaphore()
    first = [at_z(d) for d in (4, 12, 3, 13, 2, 14, 1, 15)]
    first += [at_g(j) for j in GROUP] + [at_y(d) for d in (2, 1, 3)]
    for dev in first:
        pl.semaphore_signal(barrier, inc=1, device_id=dev, device_id_type=MESH)

    loads = {}
    pairs = [
        (tok_h, tok),
        (mg_h, mg),
        (wq_h, wq),
        (wf_h, wf),
        (wi_h, wi),
        (lb_h, lb),
        (st_h, st),
        (hg_h, hg),
        (wo_h, wo),
        (rt_h, rt),
        (fg_h, fg),
        (gw_h, gw),
        (ew_h, ew),
        (wg_h, wg),
        (wu_h, wu),
        (wd_h, wd),
    ]
    for i, (src, dst) in enumerate(pairs):
        loads[i] = pltpu.make_async_copy(src, dst, lsem.at[i])
        loads[i].start()

    sends = []
    due = {}

    def post(key, src, dst, ss, sr, dev, arriving, own_ss, own_sr):
        cp = remote(src, dst, ss, sr, dev)
        cp.start()
        sends.append(cp)
        due[key] = remote(src, arriving, own_ss, own_sr, dev)

    def got(key):
        due.pop(key).wait_recv()

    for i in range(6):
        loads[i].wait()
    t32 = tok[...].astype(F32)
    normed = (
        t32 * lax.rsqrt(jnp.mean(t32 * t32, axis=-1, keepdims=True) + epsilon) * mg[...]
    ).astype(BF)
    q_pre = jnp.dot(normed, wq[...], preferred_element_type=F32)
    f_pre = jnp.dot(normed, wf[...], preferred_element_type=F32)
    value = jnp.dot(normed, wi[...], preferred_element_type=F32)
    query = q_pre * jax.nn.sigmoid(q_pre)
    forget = lb[...] + (1.0 - lb[...]) * jax.nn.sigmoid(f_pre)
    f_t = forget.T
    q_t = query.T
    loads[6].wait()
    rows = []
    for t in range(16):
        f_col = f_t[:, t : t + 1]
        new = f_col * st[t] + (1.0 - f_col) * value[t : t + 1, :]
        ns_ref[t] = new
        rows.append(jnp.sum(new * q_t[:, t : t + 1], axis=0, keepdims=True))
    readout = jnp.concatenate(rows, axis=0)
    for i in range(7, 10):
        loads[i].wait()
    head_out = (
        readout
        * lax.rsqrt(jnp.mean(readout * readout, axis=-1, keepdims=True) + epsilon)
        * hg[...]
    ).astype(BF)
    part = jnp.dot(head_out, wo[...], preferred_element_type=F32).astype(BF)
    for b in range(4):
        hp[b] = part[:, b * 256 : (b + 1) * 256]

    lane = lax.broadcasted_iota(jnp.int32, (16, 128), 1)
    nt = (((1,), (1,)), ((), ()))
    down = lax.broadcasted_iota(jnp.int32, (128, 16), 0)
    named = jnp.zeros((128, 16), F32)
    routes = rt[...]
    for k in range(6):
        named = named + jnp.where(routes[k : k + 1, :] == down, 1.0, 0.0)
    named = named.astype(BF)
    row = lax.broadcasted_iota(jnp.int32, (16, 16), 0)
    col = lax.broadcasted_iota(jnp.int32, (16, 16), 1)
    same = jnp.where(row == col, 1.0, 0.0).astype(BF)
    below = jnp.where(row > col, 1.0, 0.0).astype(BF)
    hits = lax.dot_general(same, named, nt, preferred_element_type=F32)
    before = lax.dot_general(below, named, nt, preferred_element_type=F32)
    codes = (hits * (1.0 + before)).astype(BF)

    def blocks(shape, axis):
        index = lax.broadcasted_iota(jnp.int32, shape, axis)
        p = lax.shift_right_logical(index, 4)
        half = lax.shift_right_logical(p, 1)
        dist = jnp.where((p & 1) == 1, half + 1, (16 - half) & 15)
        j = lax.shift_right_logical(index, 1) & 7
        there = ((x + lax.shift_right_logical(j, 1)) & 3) * 2 + ((c + j) & 1)
        return ((z + dist) & 15) * 8 + there, (index & 1).astype(F32) + 1.0

    expert, _ = blocks((256, 128), 0)
    along = lax.broadcasted_iota(jnp.int32, (256, 128), 1)
    sel = jnp.where(expert == along, 1.0, 0.0).astype(BF)
    _, want = blocks((256, 16), 0)
    found = lax.dot_general(sel, codes, nt, preferred_element_type=F32)
    spread = jnp.where(found == want, 1.0, 0.0).astype(BF)

    pl.semaphore_wait(barrier, 18)
    for j in GROUP:
        pl.semaphore_signal(k1, inc=1, device_id=at_g(j), device_id_type=MESH)

    for d in (2, 1, 3):
        to = lax.rem(y + d, 4)
        post(
            ("rs", d), hp.at[to], rs.at[4 - d], rs_s.at[d], rs_r.at[4 - d], at_y(d),
            rs.at[d], rs_s.at[d], rs_r.at[d],
        )
    pl.semaphore_wait(k1, 7)
    for d in (4, 12):
        pl.semaphore_signal(k2, inc=1, device_id=at_z(d), device_id_type=MESH)
    mixed = hp[y].astype(F32)
    for d in (1, 3, 2):
        got(("rs", d))
        mixed = mixed + rs[d].astype(F32)
    resident = tok[:, pl.ds(pl.multiple_of(y * 256, 256), 256)].astype(F32)
    resid = (resident + mixed.astype(BF).astype(F32)).astype(BF)
    d1[...] = resid
    d2s[...] = jnp.dot(spread, resid, preferred_element_type=F32).astype(BF)

    def rows_of(p):
        return pl.ds(p * 16, 16)

    def pair(p, j):
        return pl.ds(p * 16 + j * 2, 2)

    def block(p):
        return pl.ds(p * 16, 16)

    def sem(p, j):
        return p if p else 16 + j

    def at(p, j):
        x2 = lax.rem(x + j // 2, 4)
        c2 = lax.rem(c + j % 2, 2)
        return ((lax.rem(z + DIST[p], 16) * 4 + x2) * 2 + c2, y)

    for at_far in (False, True):
      if at_far:
        pl.semaphore_wait(k2, 2)
      for p, j in [o for o in ORDER if (o[0] > 8) == at_far]:
        remote(
            d2s.at[pair(p, j)],
            xb.at[y, pair(BACK[p], group_back(j))],
            d2_s.at[sem(p, j)],
            d2_r.at[sem(BACK[p], group_back(j))],
            at(p, j),
        ).start()
    for p, j in [(0, j) for j in range(1, 8)] + [(p, 0) for p in range(1, 16)]:
        span = block(p) if p else pair(p, j)
        both = remote(
            d2s.at[span], xb.at[y, span], d2_s.at[sem(p, j)], d2_r.at[sem(p, j)], at(p, j)
        )
        sends.append(both)
        due[("d2", p, j)] = both
    xb[y, 0:2, :] = d2s[0:2, :]

    def forward(p):
        for d in (2, 1, 3):
            post(
                ("yf", p, d), xb.at[y, rows_of(p)], xb.at[y, rows_of(p)],
                yf_s.at[p * 4 + d], yf_r.at[p * 4 + 4 - d], at_y(d),
                xb.at[lax.rem(y + d, 4), rows_of(p)], yf_s.at[p * 4 + d], yf_r.at[p * 4 + d],
            )

    for p in ARRIVE:
        for j in range(1, 8) if p == 0 else (0,):
            got(("d2", p, j))
        forward(p)

    for d in (2, 1, 3):
        post(
            ("re", d), d1, res.at[y], re_s.at[d], re_r.at[4 - d], at_y(d),
            res.at[lax.rem(y + d, 4)], re_s.at[d], re_r.at[d],
        )
    res[y] = resid

    for i in range(10, 13):
        loads[i].wait()
    gain = fg[...]
    for i in range(13, 16):
        loads[i].wait()

    def wait_rows(lo, hi):
        for p in range(lo, hi):
            for d in (1, 3, 2):
                got(("yf", p, d))

    for n, (lo, hi) in enumerate(CHUNKS):
        wait_rows(lo, hi)
        span = slice(lo * 16, hi * 16)
        a32 = jnp.concatenate([xb[b, span, :] for b in range(4)], axis=1).astype(F32)
        rows_in = (
            a32 * lax.rsqrt(jnp.mean(a32 * a32, axis=-1, keepdims=True) + epsilon) * gain
        ).astype(BF)
        gate_hidden = jnp.dot(rows_in, wg[...], preferred_element_type=F32)
        up_hidden = jnp.dot(rows_in, wu[...], preferred_element_type=F32)
        hb[y, span, :] = (gate_hidden * jax.nn.sigmoid(gate_hidden) * up_hidden).astype(BF)
        for d in (2, 1, 3):
            post(
                ("hb", n, d), hb.at[y, span], hb.at[y, span],
                hb_s.at[n * 4 + d], hb_r.at[n * 4 + 4 - d], at_y(d),
                hb.at[lax.rem(y + d, 4), span], hb_s.at[n * 4 + d], hb_r.at[n * 4 + d],
            )

    for n, (lo, hi) in enumerate(CHUNKS):
        span = slice(lo * 16, hi * 16)
        for d in (1, 3, 2):
            got(("hb", n, d))
        hidden = jnp.concatenate([hb[b, span, :] for b in range(4)], axis=1)
        pb[span, :] = jnp.dot(hidden, wd[...], preferred_element_type=F32).astype(BF)
        for p in range(hi - 1, lo - 1, -1):
            for j in (4, 5, 2, 3, 6, 7, 1, 0):
                if p or j:
                    remote(
                        pb.at[pair(p, j)],
                        rr.at[pair(BACK[p], group_back(j))],
                        r1_s.at[sem(p, j)],
                        r1_r.at[sem(BACK[p], group_back(j))],
                        at(p, j),
                    ).start()
    rr[0:2, :] = pb[0:2, :]
    for p, j in [(0, j) for j in range(1, 8)] + [(p, 0) for p in range(1, 16)]:
        span = block(p) if p else pair(p, j)
        both = remote(
            pb.at[span], rr.at[span], r1_s.at[sem(p, j)], r1_r.at[sem(p, j)], at(p, j)
        )
        sends.append(both)
        due[("r1", p, j)] = both

    for d in (1, 3, 2):
        got(("re", d))
    r32 = jnp.concatenate([res[b] for b in range(4)], axis=1).astype(F32)
    ffn_in = (
        r32 * lax.rsqrt(jnp.mean(r32 * r32, axis=-1, keepdims=True) + epsilon) * gain
    ).astype(BF)
    group_raw = jnp.exp(lax.dot_general(ffn_in, gw[...], nt, preferred_element_type=F32))
    group_prob = group_raw / jnp.sum(group_raw, axis=-1, keepdims=True)
    raw = jnp.exp(jnp.dot(ffn_in, ew[...], preferred_element_type=F32))
    member = lax.shift_right_logical(lane, 5)
    total = jnp.zeros((16, 128), F32)
    prior = jnp.zeros((16, 128), F32)
    for k in range(4):
        mine = member == k
        total = jnp.where(
            mine, jnp.sum(jnp.where(mine, raw, 0.0), axis=-1, keepdims=True), total
        )
        prior = jnp.where(mine, group_prob[:, k : k + 1], prior)
    weight = jnp.where(hits > 0.0, raw / total * prior, 0.0)
    gate = weight / jnp.sum(weight, axis=-1, keepdims=True)
    gate_hi = gate.astype(BF)
    gate_lo = (gate - gate_hi.astype(F32)).astype(BF)
    _, want_t = blocks((16, 256), 1)
    here = lax.dot_general(codes, sel, nt, preferred_element_type=F32) == want_t
    mix_hi = jnp.where(
        here, lax.dot_general(gate_hi, sel, nt, preferred_element_type=F32), 0.0
    ).astype(BF)
    mix_lo = jnp.where(
        here, lax.dot_general(gate_lo, sel, nt, preferred_element_type=F32), 0.0
    ).astype(BF)

    for p in range(16):
        for j in range(1, 8) if p == 0 else (0,):
            got(("r1", p, j))
    back = rr[...]
    mixture = jnp.dot(mix_hi, back, preferred_element_type=F32) + jnp.dot(
        mix_lo, back, preferred_element_type=F32
    )
    out_ref[...] = (d1[...].astype(F32) + mixture).astype(BF)
    for cp in sends:
        cp.wait_send()


def local(
    tokens,
    old_state,
    query_weight,
    forget_weight,
    input_weight,
    lower_bound,
    head_gain,
    out_weight,
    mix_gain,
    ffn_gain,
    group_weight,
    expert_weight,
    routes,
    gate_weight,
    up_weight,
    down_weight,
):
    operands = (
        tokens,
        old_state.reshape(16, 128, 128),
        query_weight,
        forget_weight,
        input_weight,
        lower_bound.reshape(1, 128),
        head_gain,
        out_weight,
        mix_gain.reshape(1, 1024),
        ffn_gain.reshape(1, 1024),
        group_weight.T,
        expert_weight,
        routes.T,
        gate_weight.reshape(1024, 256),
        up_weight.reshape(1024, 256),
        down_weight.reshape(1024, 256),
    )
    operands = [pltpu.with_memory_space_constraint(a, pltpu.HBM) for a in operands]
    dma = pltpu.SemaphoreType.DMA
    layer_out, new_state = pl.pallas_call(
        kernel,
        name="layer",
        out_shape=(
            jax.ShapeDtypeStruct((16, 256), BF),
            jax.ShapeDtypeStruct((16, 128, 128), F32),
        ),
        in_specs=[pl.BlockSpec(memory_space=pltpu.HBM)] * 16,
        out_specs=(pl.BlockSpec(memory_space=pltpu.VMEM),) * 2,
        scratch_shapes=[pltpu.VMEM(a.shape, a.dtype) for a in operands]
        + [
            pltpu.VMEM((4, 16, 256), BF),
            pltpu.VMEM((4, 16, 256), BF),
            pltpu.VMEM((16, 256), BF),
            pltpu.VMEM((4, 16, 256), BF),
            pltpu.VMEM((256, 256), BF),
            pltpu.VMEM((4, 256, 256), BF),
            pltpu.VMEM((4, 256, 256), BF),
            pltpu.VMEM((256, 256), BF),
            pltpu.VMEM((256, 256), BF),
            dma((16,)),
        ]
        + [dma((4,))] * 4
        + [dma((24,))] * 2
        + [dma((64,))] * 2
        + [dma((16,))] * 2
        + [dma((24,))] * 2
        + [pltpu.SemaphoreType.REGULAR] * 2,
        compiler_params=pltpu.CompilerParams(collective_id=0, has_side_effects=True, vmem_limit_bytes=16 * 1024 * 1024),
    )(*operands)
    return layer_out, new_state.reshape(16, 1, 128, 128)


def solution(mesh):
    in_specs = (
        P("ep", None),
        P("ep", "tp", None, None),
        P(None, "tp"),
        P(None, "tp"),
        P(None, "tp"),
        P("tp"),
        P("tp", None),
        P("tp", None),
        P(),
        P(),
        P(),
        P(),
        P("ep", None),
        P("ep", None, "tp"),
        P("ep", None, "tp"),
        P("ep", None, "tp"),
    )
    out_specs = (P("ep", "tp"), P("ep", "tp", None, None))
    return jax.shard_map(local, mesh=mesh, in_specs=in_specs, out_specs=out_specs, check_vma=False)
```

```python
import jax
import jax.numpy as jnp
from jax import lax
from jax.experimental import pallas as pl
from jax.experimental.pallas import tpu as pltpu
from jax.sharding import PartitionSpec as P

epsilon = 1e-06
MESH = pl.DeviceIdType.MESH
BF = jnp.bfloat16
F32 = jnp.float32

DIST = [0] + [(p + 1) // 2 if p % 2 else 16 - p // 2 for p in range(1, 16)]
BACK = [DIST.index((16 - d) % 16) for d in DIST]
FAR = list(range(15, 0, -1))
PASSED = [(p, p + 1) for p in (8, 7, 6, 5, 4, 3, 2, 1, 0, 15, 14, 13, 12, 11, 10, 9)]
CHUNKS = [(4, 9), (0, 4), (13, 16), (9, 13)]
GROUP = [4, 5, 2, 3, 6, 7, 1]


def hops(p, j):
    return min(DIST[p], 16 - DIST[p]) + min(j // 2, 4 - j // 2)


ORDER = sorted(
    [(p, j) for p in range(16) for j in range(8) if p or j], key=lambda at: -hops(*at)
)


def group_back(j):
    return ((4 - j // 2) % 4) * 2 + j % 2


def kernel(
    tok_h,
    st_h,
    wq_h,
    wf_h,
    wi_h,
    lb_h,
    hg_h,
    wo_h,
    mg_h,
    fg_h,
    gw_h,
    ew_h,
    rt_h,
    wg_h,
    wu_h,
    wd_h,
    out_ref,
    ns_ref,
    tok,
    st,
    wq,
    wf,
    wi,
    lb,
    hg,
    wo,
    mg,
    fg,
    gw,
    ew,
    rt,
    wg,
    wu,
    wd,
    hp,
    rs,
    d1,
    res,
    d2s,
    xb,
    hb,
    pb,
    rr,
    lsem,
    rs_s,
    rs_r,
    re_s,
    re_r,
    d2_s,
    d2_r,
    yf_s,
    yf_r,
    hb_s,
    hb_r,
    r1_s,
    r1_r,
    k1,
    k2,
):
    e = lax.axis_index("ep")
    y = lax.axis_index("tp")
    c = lax.rem(e, 2)
    x = lax.rem(e // 2, 4)
    z = e // 8
    g = lax.rem(e, 8)

    def at_y(d):
        return (e, lax.rem(y + d, 4))

    def at_g(j):
        x2 = lax.rem(x + j // 2, 4)
        c2 = lax.rem(c + j % 2, 2)
        return ((z * 4 + x2) * 2 + c2, y)

    def at_z(d):
        return (lax.rem(z + d, 16) * 8 + g, y)

    def remote(src, dst, ss, sr, dev):
        return pltpu.make_async_remote_copy(
            src_ref=src, dst_ref=dst, send_sem=ss, recv_sem=sr, device_id=dev, device_id_type=MESH
        )

    barrier = pltpu.get_barrier_semaphore()
    first = [at_z(d) for d in (4, 12, 3, 13, 2, 14, 1, 15)]
    first += [at_g(j) for j in GROUP] + [at_y(d) for d in (2, 1, 3)]
    for dev in first:
        pl.semaphore_signal(barrier, inc=1, device_id=dev, device_id_type=MESH)

    loads = {}
    pairs = [
        (tok_h, tok),
        (mg_h, mg),
        (wq_h, wq),
        (wf_h, wf),
        (wi_h, wi),
        (lb_h, lb),
        (st_h, st),
        (hg_h, hg),
        (wo_h, wo),
        (rt_h, rt),
        (fg_h, fg),
        (gw_h, gw),
        (ew_h, ew),
        (wg_h, wg),
        (wu_h, wu),
        (wd_h, wd),
    ]
    for i, (src, dst) in enumerate(pairs):
        loads[i] = pltpu.make_async_copy(src, dst, lsem.at[i])
        loads[i].start()

    sends = []
    due = {}

    def post(key, src, dst, ss, sr, dev, arriving, own_ss, own_sr):
        cp = remote(src, dst, ss, sr, dev)
        cp.start()
        sends.append(cp)
        due[key] = remote(src, arriving, own_ss, own_sr, dev)

    def got(key):
        due.pop(key).wait_recv()

    for i in range(6):
        loads[i].wait()
    t32 = tok[...].astype(F32)
    normed = (
        t32 * lax.rsqrt(jnp.mean(t32 * t32, axis=-1, keepdims=True) + epsilon) * mg[...]
    ).astype(BF)
    q_pre = jnp.dot(normed, wq[...], preferred_element_type=F32)
    f_pre = jnp.dot(normed, wf[...], preferred_element_type=F32)
    value = jnp.dot(normed, wi[...], preferred_element_type=F32)
    query = q_pre * jax.nn.sigmoid(q_pre)
    forget = lb[...] + (1.0 - lb[...]) * jax.nn.sigmoid(f_pre)
    f_t = forget.T
    q_t = query.T
    loads[6].wait()
    rows = []
    for t in range(16):
        f_col = f_t[:, t : t + 1]
        new = f_col * st[t] + (1.0 - f_col) * value[t : t + 1, :]
        ns_ref[t] = new
        rows.append(jnp.sum(new * q_t[:, t : t + 1], axis=0, keepdims=True))
    readout = jnp.concatenate(rows, axis=0)
    for i in range(7, 10):
        loads[i].wait()
    head_out = (
        readout
        * lax.rsqrt(jnp.mean(readout * readout, axis=-1, keepdims=True) + epsilon)
        * hg[...]
    ).astype(BF)
    part = jnp.dot(head_out, wo[...], preferred_element_type=F32).astype(BF)
    for b in range(4):
        hp[b] = part[:, b * 256 : (b + 1) * 256]

    lane = lax.broadcasted_iota(jnp.int32, (16, 128), 1)
    nt = (((1,), (1,)), ((), ()))
    down = lax.broadcasted_iota(jnp.int32, (128, 16), 0)
    named = jnp.zeros((128, 16), F32)
    routes = rt[...]
    for k in range(6):
        named = named + jnp.where(routes[k : k + 1, :] == down, 1.0, 0.0)
    named = named.astype(BF)
    row = lax.broadcasted_iota(jnp.int32, (16, 16), 0)
    col = lax.broadcasted_iota(jnp.int32, (16, 16), 1)
    same = jnp.where(row == col, 1.0, 0.0).astype(BF)
    below = jnp.where(row > col, 1.0, 0.0).astype(BF)
    hits = lax.dot_general(same, named, nt, preferred_element_type=F32)
    before = lax.dot_general(below, named, nt, preferred_element_type=F32)
    codes = (hits * (1.0 + before)).astype(BF)

    def blocks(shape, axis):
        index = lax.broadcasted_iota(jnp.int32, shape, axis)
        p = lax.shift_right_logical(index, 4)
        half = lax.shift_right_logical(p, 1)
        dist = jnp.where((p & 1) == 1, half + 1, (16 - half) & 15)
        j = lax.shift_right_logical(index, 1) & 7
        there = ((x + lax.shift_right_logical(j, 1)) & 3) * 2 + ((c + j) & 1)
        return ((z + dist) & 15) * 8 + there, (index & 1).astype(F32) + 1.0

    expert, _ = blocks((256, 128), 0)
    along = lax.broadcasted_iota(jnp.int32, (256, 128), 1)
    sel = jnp.where(expert == along, 1.0, 0.0).astype(BF)
    _, want = blocks((256, 16), 0)
    found = lax.dot_general(sel, codes, nt, preferred_element_type=F32)
    spread = jnp.where(found == want, 1.0, 0.0).astype(BF)

    pl.semaphore_wait(barrier, 18)
    for j in GROUP:
        pl.semaphore_signal(k1, inc=1, device_id=at_g(j), device_id_type=MESH)

    for d in (2, 1, 3):
        to = lax.rem(y + d, 4)
        post(
            ("rs", d), hp.at[to], rs.at[4 - d], rs_s.at[d], rs_r.at[4 - d], at_y(d),
            rs.at[d], rs_s.at[d], rs_r.at[d],
        )
    pl.semaphore_wait(k1, 7)
    for d in (4, 12):
        pl.semaphore_signal(k2, inc=1, device_id=at_z(d), device_id_type=MESH)
    mixed = hp[y].astype(F32)
    for d in (1, 3, 2):
        got(("rs", d))
        mixed = mixed + rs[d].astype(F32)
    resident = tok[:, pl.ds(pl.multiple_of(y * 256, 256), 256)].astype(F32)
    resid = (resident + mixed.astype(BF).astype(F32)).astype(BF)
    d1[...] = resid
    d2s[...] = jnp.dot(spread, resid, preferred_element_type=F32).astype(BF)

    def rows_of(p):
        return pl.ds(p * 16, 16)

    def pair(p, j):
        return pl.ds(p * 16 + j * 2, 2)

    def block(p):
        return pl.ds(p * 16, 16)

    def sem(p, j):
        return p if p else 16 + j

    def at(p, j):
        x2 = lax.rem(x + j // 2, 4)
        c2 = lax.rem(c + j % 2, 2)
        return ((lax.rem(z + DIST[p], 16) * 4 + x2) * 2 + c2, y)

    for at_far in (False, True):
      if at_far:
        pl.semaphore_wait(k2, 2)
      for p, j in [o for o in ORDER if (o[0] > 8) == at_far]:
        remote(
            d2s.at[pair(p, j)],
            xb.at[y, pair(BACK[p], group_back(j))],
            d2_s.at[sem(p, j)],
            d2_r.at[sem(BACK[p], group_back(j))],
            at(p, j),
        ).start()
    for p, j in [(0, j) for j in range(1, 8)] + [(p, 0) for p in range(1, 16)]:
        span = block(p) if p else pair(p, j)
        both = remote(
            d2s.at[span], xb.at[y, span], d2_s.at[sem(p, j)], d2_r.at[sem(p, j)], at(p, j)
        )
        sends.append(both)
        due[("d2", p, j)] = both
    xb[y, 0:2, :] = d2s[0:2, :]

    def forward(p, span):
        for d in (2, 1, 3):
            post(
                ("yf", p, d), xb.at[y, span], xb.at[y, span],
                yf_s.at[p * 4 + d], yf_r.at[p * 4 + 4 - d], at_y(d),
                xb.at[lax.rem(y + d, 4), span], yf_s.at[p * 4 + d], yf_r.at[p * 4 + d],
            )

    for lo, hi in PASSED:
        for p in range(lo, hi):
            for j in range(1, 8) if p == 0 else (0,):
                got(("d2", p, j))
        forward(lo, pl.ds(lo * 16, (hi - lo) * 16))

    for i in range(10, 13):
        loads[i].wait()
    gain = fg[...]
    for i in range(13, 16):
        loads[i].wait()

    def wait_rows(lo, hi):
        for p, _ in PASSED:
            if lo <= p < hi:
                for d in (1, 3, 2):
                    got(("yf", p, d))

    for n, (lo, hi) in enumerate(CHUNKS):
        wait_rows(lo, hi)
        span = slice(lo * 16, hi * 16)
        a32 = jnp.concatenate([xb[b, span, :] for b in range(4)], axis=1).astype(F32)
        rows_in = (
            a32 * lax.rsqrt(jnp.mean(a32 * a32, axis=-1, keepdims=True) + epsilon) * gain
        ).astype(BF)
        gate_hidden = jnp.dot(rows_in, wg[...], preferred_element_type=F32)
        up_hidden = jnp.dot(rows_in, wu[...], preferred_element_type=F32)
        hb[y, span, :] = (gate_hidden * jax.nn.sigmoid(gate_hidden) * up_hidden).astype(BF)
        for d in (2, 1, 3):
            post(
                ("hb", n, d), hb.at[y, span], hb.at[y, span],
                hb_s.at[n * 4 + d], hb_r.at[n * 4 + 4 - d], at_y(d),
                hb.at[lax.rem(y + d, 4), span], hb_s.at[n * 4 + d], hb_r.at[n * 4 + d],
            )

    for d in (2, 1, 3):
        post(
            ("re", d), d1, res.at[y], re_s.at[d], re_r.at[4 - d], at_y(d),
            res.at[lax.rem(y + d, 4)], re_s.at[d], re_r.at[d],
        )
    res[y] = resid

    for n, (lo, hi) in enumerate(CHUNKS):
        span = slice(lo * 16, hi * 16)
        for d in (1, 3, 2):
            got(("hb", n, d))
        hidden = jnp.concatenate([hb[b, span, :] for b in range(4)], axis=1)
        pb[span, :] = jnp.dot(hidden, wd[...], preferred_element_type=F32).astype(BF)
        for p in range(hi - 1, lo - 1, -1):
            for j in (4, 5, 2, 3, 6, 7, 1, 0):
                if p or j:
                    remote(
                        pb.at[pair(p, j)],
                        rr.at[pair(BACK[p], group_back(j))],
                        r1_s.at[sem(p, j)],
                        r1_r.at[sem(BACK[p], group_back(j))],
                        at(p, j),
                    ).start()
    rr[0:2, :] = pb[0:2, :]
    for p, j in [(0, j) for j in range(1, 8)] + [(p, 0) for p in range(1, 16)]:
        span = block(p) if p else pair(p, j)
        both = remote(
            pb.at[span], rr.at[span], r1_s.at[sem(p, j)], r1_r.at[sem(p, j)], at(p, j)
        )
        sends.append(both)
        due[("r1", p, j)] = both

    for d in (1, 3, 2):
        got(("re", d))
    r32 = jnp.concatenate([res[b] for b in range(4)], axis=1).astype(F32)
    ffn_in = (
        r32 * lax.rsqrt(jnp.mean(r32 * r32, axis=-1, keepdims=True) + epsilon) * gain
    ).astype(BF)
    group_raw = jnp.exp(lax.dot_general(ffn_in, gw[...], nt, preferred_element_type=F32))
    group_prob = group_raw / jnp.sum(group_raw, axis=-1, keepdims=True)
    raw = jnp.exp(jnp.dot(ffn_in, ew[...], preferred_element_type=F32))
    member = lax.shift_right_logical(lane, 5)
    total = jnp.zeros((16, 128), F32)
    prior = jnp.zeros((16, 128), F32)
    for k in range(4):
        mine = member == k
        total = jnp.where(
            mine, jnp.sum(jnp.where(mine, raw, 0.0), axis=-1, keepdims=True), total
        )
        prior = jnp.where(mine, group_prob[:, k : k + 1], prior)
    weight = jnp.where(hits > 0.0, raw / total * prior, 0.0)
    gate = weight / jnp.sum(weight, axis=-1, keepdims=True)
    gate_hi = gate.astype(BF)
    gate_lo = (gate - gate_hi.astype(F32)).astype(BF)
    _, want_t = blocks((16, 256), 1)
    here = lax.dot_general(codes, sel, nt, preferred_element_type=F32) == want_t
    mix_hi = jnp.where(
        here, lax.dot_general(gate_hi, sel, nt, preferred_element_type=F32), 0.0
    ).astype(BF)
    mix_lo = jnp.where(
        here, lax.dot_general(gate_lo, sel, nt, preferred_element_type=F32), 0.0
    ).astype(BF)

    for p in range(16):
        for j in range(1, 8) if p == 0 else (0,):
            got(("r1", p, j))
    back = rr[...]
    mixture = jnp.dot(mix_hi, back, preferred_element_type=F32) + jnp.dot(
        mix_lo, back, preferred_element_type=F32
    )
    out_ref[...] = (d1[...].astype(F32) + mixture).astype(BF)
    for cp in sends:
        cp.wait_send()


def store(out_ref, ns_ref, out_h, ns_h, sems):
    copies = [pltpu.make_async_copy(out_ref, out_h, sems.at[4])]
    for i in range(4):
        span = pl.ds(i * 4, 4)
        copies.append(pltpu.make_async_copy(ns_ref.at[span], ns_h.at[span], sems.at[i]))
    for cp in copies:
        cp.start()
    for cp in copies:
        cp.wait()


def local(
    tokens,
    old_state,
    query_weight,
    forget_weight,
    input_weight,
    lower_bound,
    head_gain,
    out_weight,
    mix_gain,
    ffn_gain,
    group_weight,
    expert_weight,
    routes,
    gate_weight,
    up_weight,
    down_weight,
):
    operands = (
        tokens,
        old_state.reshape(16, 128, 128),
        query_weight,
        forget_weight,
        input_weight,
        lower_bound.reshape(1, 128),
        head_gain,
        out_weight,
        mix_gain.reshape(1, 1024),
        ffn_gain.reshape(1, 1024),
        group_weight.T,
        expert_weight,
        routes.T,
        gate_weight.reshape(1024, 256),
        up_weight.reshape(1024, 256),
        down_weight.reshape(1024, 256),
    )
    operands = [pltpu.with_memory_space_constraint(a, pltpu.HBM) for a in operands]
    dma = pltpu.SemaphoreType.DMA
    layer_out, new_state = pl.pallas_call(
        kernel,
        name="layer",
        out_shape=(
            jax.ShapeDtypeStruct((16, 256), BF),
            jax.ShapeDtypeStruct((16, 128, 128), F32),
        ),
        in_specs=[pl.BlockSpec(memory_space=pltpu.HBM)] * 16,
        out_specs=(pl.BlockSpec(memory_space=pltpu.VMEM),) * 2,
        scratch_shapes=[pltpu.VMEM(a.shape, a.dtype) for a in operands]
        + [
            pltpu.VMEM((4, 16, 256), BF),
            pltpu.VMEM((4, 16, 256), BF),
            pltpu.VMEM((16, 256), BF),
            pltpu.VMEM((4, 16, 256), BF),
            pltpu.VMEM((256, 256), BF),
            pltpu.VMEM((4, 256, 256), BF),
            pltpu.VMEM((4, 256, 256), BF),
            pltpu.VMEM((256, 256), BF),
            pltpu.VMEM((256, 256), BF),
            dma((16,)),
        ]
        + [dma((4,))] * 4
        + [dma((24,))] * 2
        + [dma((64,))] * 2
        + [dma((16,))] * 2
        + [dma((24,))] * 2
        + [pltpu.SemaphoreType.REGULAR] * 2,
        compiler_params=pltpu.CompilerParams(collective_id=0, has_side_effects=True, vmem_limit_bytes=16 * 1024 * 1024),
    )(*operands)
    layer_out, new_state = pl.pallas_call(
        store,
        name="store",
        out_shape=(
            jax.ShapeDtypeStruct((16, 256), BF),
            jax.ShapeDtypeStruct((16, 128, 128), F32),
        ),
        in_specs=[pl.BlockSpec(memory_space=pltpu.VMEM)] * 2,
        out_specs=(pl.BlockSpec(memory_space=pltpu.HBM),) * 2,
        scratch_shapes=[dma((5,))],
        compiler_params=pltpu.CompilerParams(vmem_limit_bytes=4 * 1024 * 1024),
    )(layer_out, new_state)
    return layer_out, new_state.reshape(16, 1, 128, 128)


def solution(mesh):
    in_specs = (
        P("ep", None),
        P("ep", "tp", None, None),
        P(None, "tp"),
        P(None, "tp"),
        P(None, "tp"),
        P("tp"),
        P("tp", None),
        P("tp", None),
        P(),
        P(),
        P(),
        P(),
        P("ep", None),
        P("ep", None, "tp"),
        P("ep", None, "tp"),
        P("ep", None, "tp"),
    )
    out_specs = (P("ep", "tp"), P("ep", "tp", None, None))
    return jax.shard_map(local, mesh=mesh, in_specs=in_specs, out_specs=out_specs, check_vma=False)
```
